32 devices in a mesh: sp: 8 (over z, core), tp: 4 (over y, x).
Axes of the slice: x: 2, y: 2, z: 4, core: 2. Of those that a mesh axis runs over, the one named last changes fastest.
Arguments:
- tokens: bfloat16 [2, 6144, 4096], P(None, 'sp', 'tp'), may hold values from -6 to 6
- w_key: bfloat16 [4096, 2048], P(None, 'tp'), may hold values from -0.09375 to 0.09375
- w_value: bfloat16 [4096, 2048], P(None, 'tp'), may hold values from -0.09375 to 0.09375
- w_gate: bfloat16 [4096, 4, 16], replicated, may hold values from -0.09375 to 0.09375
- forget_bias: float32 [2, 16], replicated, may hold values from 3.9 to 13, as said below
- log_shift: float32 [2, 4, 16, 6144], P(None, None, 'tp', 'sp'), may hold values from -5 to 121, as said below
- new_query: bfloat16 [2, 1024, 2048], P(None, 'sp', 'tp'), may hold values from -6 to 6
Outputs:
- cache_matrix: bfloat16 [2, 2, 16, 128, 128], P(None, None, 'tp')
- cache_norm: float32 [2, 2, 16, 128], P(None, None, 'tp')
- cache_max: float32 [2, 2, 16], P(None, None, 'tp')
- first_read: bfloat16 [2, 1024, 2048], P(None, 'sp', 'tp')
The draws below stay inside these ranges and needn't reach their ends.
Inputs may be any that keep to these rules, and one draw needn't show every extreme that they name: `forget_bias`: added to the forget gates' pre-activations, by direction and head. `log_shift`: rows 0 and 2 are added to the input gates of the two directions; rows 1 and 3 are added to the log forget gates and are never positive.
All inputs are finite; a program needn't handle non-finite values.
Results may differ from the reference program's by a relative error of at most 0.024.
Values may be sent and summed in bfloat16 or wider, within the bound.
A program may use at most 64 MiB of HBM per device.

```python
import math
import jax
import jax.numpy as jnp
from jax import lax

D = 4096
HEADS = 16
HEAD = 128
SEQS = 2
SEG = 768
CONTEXT_SPAN = 6144
NEW = 1024


def draw_forget_bias(key, part):
    pick_key, fast_key, slow_key = jax.random.split(jax.random.fold_in(key, 7), 3)
    slow_share = 0.5
    is_slow = jax.random.uniform(pick_key, (2, HEADS)) < slow_share
    fast_value = jax.random.uniform(fast_key, (2, HEADS), minval=3.9, maxval=5.0)
    slow_value = math.log(CONTEXT_SPAN) + 2.0 + jax.random.uniform(slow_key, (2, HEADS), minval=0.0, maxval=0.5)
    return jnp.where(is_slow, slow_value, fast_value).astype(jnp.float32)


def draw_log_shift(key, part):
    parallel_texts = jax.random.split(jax.random.fold_in(key, 13), 6)
    array_dimensions = (SEQS, 4, HEADS, CONTEXT_SPAN)
    inputs = jnp.clip(jax.random.normal(parallel_texts[0], array_dimensions), -4.0, 4.0)
    shrink_factor = jnp.exp(jax.random.uniform(parallel_texts[3], (SEQS, 1, HEADS, CONTEXT_SPAN // SEG), minval=math.log(0.25), maxval=0.0))
    shrink_factor = jnp.repeat(shrink_factor, SEG, axis=3)
    span_of_batch = jax.random.uniform(parallel_texts[4], array_dimensions) < 2.0 / CONTEXT_SPAN
    layer_stack_count = jax.random.uniform(parallel_texts[5], array_dimensions, minval=0.22, maxval=0.69)
    retention_switch = -shrink_factor / CONTEXT_SPAN - jnp.where(span_of_batch, layer_stack_count, 0.0)
    is_forget = (jnp.arange(4) % 2 == 1)[None, :, None, None]
    return jnp.where(is_forget, retention_switch, inputs).astype(jnp.float32)


def shard_levels(key, dims, cuts, least, top_value):
    gain, own = 1.0, jax.random.fold_in(key, 6)
    for dim, shards_of in cuts:
        steps = jnp.exp(jax.random.uniform(jax.random.fold_in(own, dim), (shards_of,), jnp.float32, least / len(cuts), top_value / len(cuts)))
        gain = gain * jnp.repeat(steps, dims[dim] // shards_of).reshape([-1 if axis == dim else 1 for axis in range(len(dims))])
    return gain


def scatter_about(rng, shape, spread, reach, cuts=(), kind=jnp.bfloat16):
    values = spread * jax.random.normal(rng, shape, jnp.float32)
    if cuts:
        values = values * shard_levels(rng, shape, cuts, -0.22, 0.18)
    return jnp.clip(values, -reach, reach).astype(kind)


def setup_inputs(seed: int = 0) -> dict:
    arg_keys = jax.random.split(jax.random.key(seed), 8)
    return {
        "tokens": scatter_about(arg_keys[0], (SEQS, CONTEXT_SPAN, D), 1.0, 6.0, ((1, 8), (2, 4))),
        "w_key": scatter_about(arg_keys[1], (D, HEADS * HEAD), D ** -0.5, 0.09375, ((1, 4),)),
        "w_value": scatter_about(arg_keys[2], (D, HEADS * HEAD), D ** -0.5, 0.09375, ((1, 4),)),
        "w_gate": scatter_about(arg_keys[3], (D, 4, HEADS), D ** -0.5, 0.09375),
        "forget_bias": draw_forget_bias(jax.random.fold_in(arg_keys[7], 71), 0),
        "log_shift": draw_log_shift(jax.random.fold_in(arg_keys[7], 71), 0),
        "new_query": scatter_about(arg_keys[6], (SEQS, NEW, HEADS * HEAD), 1.0, 6.0, ((1, 8), (2, 4))),
    }


def reference(tokens, w_key, w_value, w_gate, forget_bias, log_shift, new_query):
    flat_tokens = tokens.reshape(SEQS * CONTEXT_SPAN, D)
    key_rows = jnp.dot(flat_tokens, w_key, preferred_element_type=jnp.float32).astype(jnp.bfloat16)
    key_rows = key_rows.reshape(SEQS, CONTEXT_SPAN, HEADS, HEAD)
    value_rows = jnp.dot(flat_tokens, w_value, preferred_element_type=jnp.float32).astype(jnp.bfloat16)
    value_rows = value_rows.reshape(SEQS, CONTEXT_SPAN, HEADS, HEAD)
    gate_rows = jnp.dot(flat_tokens, w_gate.reshape(D, 4 * HEADS), preferred_element_type=jnp.float32)
    gate_rows = gate_rows.reshape(SEQS, CONTEXT_SPAN, 4, HEADS).transpose(0, 2, 3, 1)
    input_fwd = gate_rows[:, 0] + log_shift[:, 0]
    forget_fwd = jax.nn.log_sigmoid(gate_rows[:, 1] + forget_bias[0][None, :, None]) + log_shift[:, 1]
    input_bwd = gate_rows[:, 2] + log_shift[:, 2]
    forget_bwd = jax.nn.log_sigmoid(gate_rows[:, 3] + forget_bias[1][None, :, None]) + log_shift[:, 3]
    climb_fwd = jnp.cumsum(forget_fwd, axis=-1)
    total_fwd = climb_fwd[..., -1]
    weight_fwd = total_fwd[..., None] - climb_fwd + input_fwd
    climb_bwd = jnp.cumsum(forget_bwd, axis=-1)
    total_bwd = climb_bwd[..., -1]
    weight_bwd = climb_bwd - forget_bwd + input_bwd
    weights = jnp.stack([weight_fwd, weight_bwd], axis=1)
    totals = jnp.stack([total_fwd, total_bwd], axis=1)
    cache_max = jnp.maximum(totals, jnp.max(weights, axis=-1))
    scale_now = jnp.exp(weights - cache_max[..., None])
    key_f = key_rows.astype(jnp.float32).transpose(0, 2, 1, 3) * (HEAD ** -0.5)
    value_f = value_rows.astype(jnp.float32).transpose(0, 2, 1, 3)
    cache_norm = jnp.einsum('bjhl,bhld->bjhd', scale_now, key_f, precision=lax.Precision.HIGHEST)
    matrices = []
    for direction in range(2):
        weighted = scale_now[:, direction, :, :, None] * key_f
        matrices.append(jnp.einsum('bhld,bhle->bhde', weighted, value_f, precision=lax.Precision.HIGHEST))
    cache_matrix = jnp.stack(matrices, axis=1).astype(jnp.bfloat16)
    queries = new_query.reshape(SEQS, NEW, HEADS, HEAD).astype(jnp.float32)
    numerator = jnp.einsum('bthd,bjhde->bjthe', queries, cache_matrix.astype(jnp.float32))
    denominator = jnp.einsum('bthd,bjhd->bjth', queries, cache_norm, precision=lax.Precision.HIGHEST)
    divisor = jnp.maximum(jnp.abs(denominator), 1.0)
    first_read = jnp.sum(numerator / divisor[..., None], axis=1)
    first_read = first_read.reshape(SEQS, NEW, HEADS * HEAD).astype(jnp.bfloat16)
    return cache_matrix, cache_norm, cache_max, first_read
```

```python
import functools

import jax
import jax.numpy as jnp
from jax import lax
from jax.experimental import pallas as pl
from jax.experimental.pallas import tpu as pltpu
from jax.sharding import PartitionSpec as P

HEAD = 128
CORES = 2
BF = jnp.bfloat16
F32 = jnp.float32
MESH = pl.DeviceIdType.MESH


def kernel(
    n_sp, n_tp, per_head, pad,
    tok_in, wk_in, wv_in, shift_in, wg, bias, query,
    cm_out, norm_out, max_out, read_out,
    tok, wk, wv, pk, pv, shift, shift_in2, shift_all, acc_k, acc_v, gates, kp, vp,
    stats, stat_own, norms, norm_own, pair_in, pair_own, st, rs, final, cm,
    tok_sem, wk_sem, wv_sem, local_sem, shift_sem, stat_sem, norm_sem, pair_sem, rs_sem, cm_sem,
    send_sem,
):
    s = lax.axis_index("sp")
    t = lax.axis_index("tp")
    half = n_tp // 2
    prompt = t // half
    other = 1 - prompt
    mate = lax.rem(t + half, n_tp)
    z, core = s // CORES, lax.rem(s, CORES)
    n_z = n_sp // CORES
    seg, width = tok.shape[1], tok.shape[2]
    depth = pk.shape[1]
    cols = wk.shape[2]
    sends = []
    count = [0]

    def remote(src, dst, recv, sp_to, tp_to):
        k = count[0]
        count[0] += 1
        return pltpu.make_async_remote_copy(
            src_ref=src, dst_ref=dst, send_sem=send_sem.at[k], recv_sem=recv,
            device_id=(sp_to, tp_to), device_id_type=MESH,
        )

    def send(src, dst, recv, sp_to, tp_to):
        copy = remote(src, dst, recv, sp_to, tp_to)
        copy.start()
        sends.append((None, copy))

    def send_if(cond, src, dst, recv, sp_to, tp_to):
        copy = remote(src, dst, recv, sp_to, tp_to)

        @pl.when(cond)
        def _():
            copy.start()

        sends.append((cond, copy))

    def arrived(ref, sem):
        pltpu.make_async_copy(ref, ref, sem).wait()

    barrier = pltpu.get_barrier_semaphore()
    greeted = 0
    for d in range(1, n_tp):
        pl.semaphore_signal(barrier, inc=1, device_id=(s, lax.rem(t + d, n_tp)), device_id_type=MESH)
        greeted += 1
    for d in range(1, n_sp):
        for column in (t, mate):
            pl.semaphore_signal(
                barrier, inc=1, device_id=(lax.rem(s + d, n_sp), column), device_id_type=MESH
            )
            greeted += 1

    loads = []

    def load(src, dst):
        copy = pltpu.make_async_copy(src, dst, local_sem.at[len(loads)])
        copy.start()
        loads.append(copy)

    load(tok_in.at[prompt], tok.at[t])
    load(wk_in, wk)
    load(wv_in, wv)
    load(shift_in.at[prompt], shift)
    pl.semaphore_wait(barrier, greeted)

    rows = seg // 2
    send(wk_in.at[s], pk.at[s], wk_sem.at[s], s, mate)
    send(shift_in.at[other], shift_in2, shift_sem, s, mate)
    peers = [prompt * half + lax.rem(t + d, half) for d in range(1, half)]
    for part in range(2):
        span = pl.ds(part * rows, rows)
        send(tok_in.at[other, span], tok.at[t, span], tok_sem.at[t, part], s, mate)
        for peer in peers:
            send(tok_in.at[prompt, span], tok.at[t, span], tok_sem.at[t, part], s, peer)
        if part == 0:
            send(wv_in.at[s], pv.at[s], wv_sem.at[s], s, mate)

    def relay_tokens(part):
        span = pl.ds(part * rows, rows)
        arrived(tok.at[mate, span], tok_sem.at[mate, part])
        for peer in peers:
            send(tok.at[mate, span], tok.at[mate, span], tok_sem.at[mate, part], s, peer)

    sibling = z * CORES + 1 - core

    def own_slice(held, sem):
        arrived(held.at[s], sem.at[s])
        up, down = jnp.minimum(z + 1, n_z - 1), jnp.maximum(z - 1, 0)
        send_if(z + 1 < n_z, held.at[s], held.at[s], sem.at[s], up * CORES + core, t)
        send_if(z > 0, held.at[s], held.at[s], sem.at[s], down * CORES + core, t)
        send(held.at[s], held.at[s], sem.at[s], sibling, t)

    def chain(held, sem, k):
        up, down = jnp.minimum(z + 1, n_z - 1), jnp.maximum(z - 1, 0)
        low = z - 1 - k
        low_at = jnp.maximum(low, 0) * CORES + core
        high = z + 1 + k
        high_at = jnp.minimum(high, n_z - 1) * CORES + core

        @pl.when(low >= 0)
        def _():
            arrived(held.at[low_at], sem.at[low_at])

        send_if((low >= 0) & (z + 1 < n_z), held.at[low_at], held.at[low_at], sem.at[low_at], up * CORES + core, t)
        send_if(low >= 0, held.at[low_at], held.at[low_at], sem.at[low_at], sibling, t)

        @pl.when(high < n_z)
        def _():
            arrived(held.at[high_at], sem.at[high_at])

        send_if((high < n_z) & (z > 0), held.at[high_at], held.at[high_at], sem.at[high_at], down * CORES + core, t)
        send_if(high < n_z, held.at[high_at], held.at[high_at], sem.at[high_at], sibling, t)

    tile = 256 if seg % 256 == 0 else seg
    tiles = seg // tile
    per_slot = width // depth if width >= depth else 1

    def weight_rows(ref, q):
        if width >= depth:
            return ref[pl.ds(q * per_slot, per_slot)].reshape(width, cols)
        share = depth // width
        return ref[q // share, pl.ds(pl.multiple_of(lax.rem(q, share) * width, width), width), :]

    def project(q, first):
        @pl.loop(0, tiles)
        def _(i):
            span = pl.ds(pl.multiple_of(i * tile, tile), tile)
            x = tok[q, span, :]
            ak = jnp.dot(x, weight_rows(wk, q), preferred_element_type=F32)
            av = jnp.dot(x, weight_rows(wv, q), preferred_element_type=F32)
            if first:
                acc_k[span, :] = ak
                acc_v[span, :] = av
            else:
                acc_k[span, :] += ak
                acc_v[span, :] += av

        g = lax.dot_general(wg[q], tok[q], (((1,), (1,)), ((), ())), preferred_element_type=F32)
        gates[...] = g if first else gates[...] + g

    for copy in loads:
        copy.wait()
    project(t, True)

    def peer_tokens(q):
        for part in range(2):
            span = pl.ds(part * rows, rows)
            arrived(tok.at[q, span], tok_sem.at[q, part])
        project(q, False)

    own_slice(pk, wk_sem)
    mid = [("k", k) for k in range(n_z - 1)]
    if mid:
        chain(pk, wk_sem, mid[0][1])
    relay_tokens(0)
    for _, k in mid[1:2]:
        chain(pk, wk_sem, k)
    own_slice(pv, wv_sem)
    for _, k in mid[2:]:
        chain(pk, wk_sem, k)
    for peer in peers:
        peer_tokens(peer)
    for _, k in mid[0:1]:
        chain(pv, wv_sem, k)
    relay_tokens(1)
    project(mate, False)
    for _, k in mid[1:2]:
        chain(pv, wv_sem, k)
    for peer in peers:
        peer_tokens(lax.rem(peer + half, n_tp))

    arrived(shift_in2, shift_sem)
    shift_all[...] = jnp.zeros_like(shift_all)
    for g in range(4):
        shift_all[g, 0:per_head, :] = shift[g]
        shift_all[g, per_head : 2 * per_head, :] = shift_in2[g]

    lane = lax.broadcasted_iota(jnp.int32, (pad, seg), 1)

    def log_sigmoid(v):
        return jnp.minimum(v, 0.0) - jnp.log1p(jnp.exp(-jnp.abs(v)))

    def climb(v):
        step = 1
        while step < seg:
            v = v + jnp.where(lane >= step, pltpu.roll(v, step, 1), 0.0)
            step *= 2
        return v

    def gate(g):
        return gates[g * pad : (g + 1) * pad, :]

    in_f = gate(0) + shift_all[0]
    fo_f = log_sigmoid(gate(1) + bias[0][:, 0:1]) + shift_all[1]
    in_b = gate(2) + shift_all[2]
    fo_b = log_sigmoid(gate(3) + bias[1][:, 0:1]) + shift_all[3]
    total_f = jnp.sum(fo_f, axis=1, keepdims=True)
    total_b = jnp.sum(fo_b, axis=1, keepdims=True)
    w_f = total_f - climb(fo_f) + in_f
    w_b = climb(fo_b) - fo_b + in_b
    top_f = jnp.max(w_f, axis=1, keepdims=True)
    top_b = jnp.max(w_b, axis=1, keepdims=True)
    first_lane = lax.broadcasted_iota(jnp.int32, (pad, HEAD), 1) == 0
    stat_own[0] = jnp.where(first_lane, top_f, total_f)
    stat_own[1] = jnp.where(first_lane, top_b, total_b)
    for d in range(1, n_sp):
        to = lax.rem(s + d, n_sp)
        send(stat_own, stats.at[s], stat_sem.at[s], to, t)

    def far(held, dest):
        @pl.loop(0, tiles)
        def _(i):
            span = pl.ds(pl.multiple_of(i * tile, tile), tile)
            total = jnp.zeros((tile, cols), F32)
            for q in range(n_tp):
                total += jnp.dot(tok[q, span, :], weight_rows(held, q), preferred_element_type=F32)
            dest[span, :] = total.astype(BF)

    for k in range(n_z):
        got = k * CORES + 1 - core
        arrived(pk.at[got], wk_sem.at[got])
    far(pk, kp)
    for _, k in mid[2:]:
        chain(pv, wv_sem, k)

    stats[s] = stat_own[...]
    for d in range(1, n_sp):
        frm = lax.rem(s + d, n_sp)
        arrived(stats.at[frm], stat_sem.at[frm])

    everyone = [stats[k] for k in range(n_sp)]
    total_all = [0.0, 0.0]
    after = [None] * n_sp
    running = jnp.zeros((pad, 1), F32)
    for k in reversed(range(n_sp)):
        after[k] = running
        running = running + everyone[k][0][:, 1:2]
    total_all[0] = running
    before = [None] * n_sp
    running = jnp.zeros((pad, 1), F32)
    for k in range(n_sp):
        before[k] = running
        running = running + everyone[k][1][:, 1:2]
    total_all[1] = running
    max_f, max_b = total_all
    passed_f = jnp.zeros((pad, 1), F32)
    passed_b = jnp.zeros((pad, 1), F32)
    for k in range(n_sp):
        max_f = jnp.maximum(max_f, everyone[k][0][:, 0:1] + after[k])
        max_b = jnp.maximum(max_b, everyone[k][1][:, 0:1] + before[k])
        passed_f = jnp.where(s == k, after[k], passed_f)
        passed_b = jnp.where(s == k, before[k], passed_b)
    scale_f = jnp.exp(w_f + (passed_f - max_f)) * HEAD**-0.5
    scale_b = jnp.exp(w_b + (passed_b - max_b)) * HEAD**-0.5
    both = jnp.concatenate([scale_f, scale_b], axis=0)
    scale_hi = both.astype(BF)
    scale_lo = (both - scale_hi.astype(F32)).astype(BF)

    block = st.shape[0] // n_sp
    row_of = lax.broadcasted_iota(jnp.int32, (2 * pad, HEAD), 0)
    norm_own[...] = jnp.zeros_like(norm_own)

    def head_state(index, k_h, v_h):
        k_t = k_h.astype(F32).T
        both_t = jnp.concatenate(
            [k_t * scale_f[index : index + 1, :], k_t * scale_b[index : index + 1, :]], axis=0
        ).astype(BF)
        st[index * 2 * HEAD : (index + 1) * 2 * HEAD, :] = jnp.dot(
            both_t, v_h, preferred_element_type=F32
        ).astype(BF)
        n = jnp.dot(scale_hi, k_h, preferred_element_type=F32) + jnp.dot(
            scale_lo, k_h, preferred_element_type=F32
        )
        mine = (row_of == index) | (row_of == index + pad)
        norm_own[...] = jnp.where(mine, n, norm_own[...])

    def scatter(side):
        for k in range(n_sp // 2):
            owner = side * (n_sp // 2) + k
            send_if(
                s != owner,
                st.at[pl.ds(owner * block, block)],
                rs.at[s], rs_sem.at[s], jnp.where(s == owner, sibling, owner), t,
            )

    for h in range(per_head):
        at = slice(h * HEAD, (h + 1) * HEAD)
        head_state(h, acc_k[:, at].astype(BF), acc_v[:, at].astype(BF))
    scatter(0)

    for k in range(n_z):
        got = k * CORES + 1 - core
        arrived(pv.at[got], wv_sem.at[got])
    far(pv, vp)
    for h in range(per_head):
        at = slice(h * HEAD, (h + 1) * HEAD)
        head_state(per_head + h, kp[:, at], vp[:, at])
    scatter(1)
    for d in range(1, n_sp):
        to = lax.rem(s + d, n_sp)
        send(norm_own, norms.at[s], norm_sem.at[s], to, t)
    norms[s] = norm_own[...]

    summed = st[pl.ds(pl.multiple_of(s * block, block), block), :].astype(F32)
    for d in range(1, n_sp):
        frm = lax.rem(s + d, n_sp)
        arrived(rs.at[frm], rs_sem.at[frm])
        summed = summed + rs[frm].astype(F32)
    final[...] = summed.astype(BF)

    piece = min(block, HEAD)
    mine_side = s < n_sp // 2
    column = jnp.where(mine_side, t, mate)
    for c in range(block // piece):
        start = s * block + c * piece
        head = lax.rem(start // (2 * HEAD), per_head)
        direction = lax.rem(start // HEAD, 2)
        inner = pl.ds(pl.multiple_of(lax.rem(start, HEAD), piece), piece)
        src = final.at[pl.ds(c * piece, piece)]
        dst = cm.at[prompt, direction, head, inner]
        for d in range(1, n_sp):
            send(src, dst, cm_sem.at[prompt], lax.rem(s + d, n_sp), column)
        keep = pltpu.make_async_copy(src, dst, cm_sem.at[prompt])

        @pl.when(mine_side)
        def _():
            keep.start()

        send_if(jnp.logical_not(mine_side), src, dst, cm_sem.at[prompt], s, mate)

    total_norm = jnp.zeros((2 * pad, HEAD), F32)
    for d in range(1, n_sp):
        frm = lax.rem(s + d, n_sp)
        arrived(norms.at[frm], norm_sem.at[frm])
    for k in range(n_sp):
        total_norm = total_norm + norms[k]
    pair_own[0] = total_norm
    pair_own[1, 0:pad, :] = jnp.broadcast_to(max_f, (pad, HEAD))
    pair_own[1, pad : 2 * pad, :] = jnp.broadcast_to(max_b, (pad, HEAD))
    send(pair_own, pair_in, pair_sem, s, mate)
    for j in range(2):
        norm_out[prompt, j] = pair_own[0, j * pad : j * pad + per_head, :]
        max_out[prompt, j] = pair_own[1, j * pad : j * pad + per_head, :]
    arrived(pair_in, pair_sem)
    for j in range(2):
        lo = j * pad + per_head
        norm_out[other, j] = pair_in[0, lo : lo + per_head, :]
        max_out[other, j] = pair_in[1, lo : lo + per_head, :]

    for b in range(2):
        arrived(cm.at[b], cm_sem.at[b])
    store = pltpu.make_async_copy(cm, cm_out, local_sem.at[len(loads)])
    store.start()
    for b in range(2):
        for h in range(per_head):
            at = slice(h * HEAD, (h + 1) * HEAD)
            q = query[b, :, at]
            q_f = q.astype(F32)
            total = jnp.zeros(q_f.shape, F32)
            for j in range(2):
                num = jnp.dot(q, cm[b, j, h], preferred_element_type=F32)
                den = jnp.sum(q_f * norm_out[b, j, h : h + 1, :], axis=1, keepdims=True)
                total = total + num / jnp.maximum(jnp.abs(den), 1.0)
            read_out[b, :, at] = total.astype(BF)

    for cond, copy in sends:
        if cond is None:
            copy.wait_send()
        else:
            pl.when(cond)(copy.wait_send)
    store.wait()


def on_device(n_sp, n_tp, tokens, w_key, w_value, w_gate, forget_bias, log_shift, new_query):
    seqs, seg, width = tokens.shape
    depth_all, cols = w_key.shape
    per_head = cols // HEAD
    pad = -(-2 * per_head // 8) * 8
    t = lax.axis_index("tp")
    mate = lax.rem(t + n_tp // 2, n_tp)

    def pair(array, axis):
        parts = [
            lax.dynamic_slice_in_dim(array, k * per_head, per_head, axis) for k in (t, mate)
        ]
        widths = [(0, 0)] * array.ndim
        widths[axis] = (0, pad - 2 * per_head)
        return jnp.pad(jnp.concatenate(parts, axis=axis), widths)

    gate_cols = pair(w_gate, 2).reshape(n_tp, width, 4 * pad).transpose(0, 2, 1)
    bias = jnp.broadcast_to(pair(forget_bias, 1)[..., None], (2, pad, HEAD))
    depth = depth_all // n_sp
    slabs = (n_sp, depth, cols)
    state_rows = 2 * per_head * 2 * HEAD
    block = state_rows // n_sp
    n_z = n_sp // CORES
    half = n_tp // 2
    n_send = (
        2 + 2 * half + 1 + 2 * (half - 1) + 2 * 3 + 2 * (n_z - 1) * 4
        + 3 * (n_sp - 1) + n_sp + max(1, block // HEAD) * n_sp + 4
    )
    vmem = pltpu.VMEM
    dma = pltpu.SemaphoreType.DMA
    new = new_query.shape[1]
    any_spec = pl.BlockSpec(memory_space=pl.ANY)
    vm_spec = pl.BlockSpec(memory_space=vmem)
    cm, norm, top, read = pl.pallas_call(
        functools.partial(kernel, n_sp, n_tp, per_head, pad),
        out_shape=(
            jax.ShapeDtypeStruct((seqs, 2, per_head, HEAD, HEAD), BF),
            jax.ShapeDtypeStruct((seqs, 2, per_head, HEAD), F32),
            jax.ShapeDtypeStruct((seqs, 2, per_head, HEAD), F32),
            jax.ShapeDtypeStruct((seqs, new, cols), BF),
        ),
        in_specs=[any_spec] * 4 + [vm_spec] * 3,
        out_specs=(any_spec, vm_spec, vm_spec, vm_spec),
        scratch_shapes=[
            vmem((n_tp, seg, width), BF),
            vmem(slabs, BF), vmem(slabs, BF), vmem(slabs, BF), vmem(slabs, BF),
            vmem((4, per_head, seg), F32), vmem((4, per_head, seg), F32), vmem((4, pad, seg), F32),
            vmem((seg, cols), F32), vmem((seg, cols), F32), vmem((4 * pad, seg), F32),
            vmem((seg, cols), BF), vmem((seg, cols), BF),
            vmem((n_sp, 2, pad, HEAD), F32), vmem((2, pad, HEAD), F32),
            vmem((n_sp, 2 * pad, HEAD), F32), vmem((2 * pad, HEAD), F32),
            vmem((2, 2 * pad, HEAD), F32), vmem((2, 2 * pad, HEAD), F32),
            vmem((state_rows, HEAD), BF), vmem((n_sp, block, HEAD), BF), vmem((block, HEAD), BF),
            vmem((seqs, 2, per_head, HEAD, HEAD), BF),
            dma((n_tp, 2)), dma((n_sp,)), dma((n_sp,)), dma((6,)), dma, dma((n_sp,)), dma((n_sp,)),
            dma, dma((n_sp,)), dma((2,)), dma((n_send,)),
        ],
        compiler_params=pltpu.CompilerParams(
            collective_id=0, has_side_effects=True, vmem_limit_bytes=60 * 2**20
        ),
    )(
        tokens, w_key.reshape(slabs), w_value.reshape(slabs), log_shift, gate_cols, bias, new_query
    )
    return cm, norm, top[..., 0], read


def solution(mesh):
    return jax.shard_map(
        functools.partial(on_device, mesh.shape["sp"], mesh.shape["tp"]),
        mesh=mesh,
        in_specs=(
            P(None, "sp", "tp"),
            P(None, "tp"),
            P(None, "tp"),
            P(),
            P(),
            P(None, None, "tp", "sp"),
            P(None, "sp", "tp"),
        ),
        out_specs=(
            P(None, None, "tp", None, None),
            P(None, None, "tp", None),
            P(None, None, "tp"),
            P(None, "sp", "tp"),
        ),
        check_vma=False,
    )
```

```python
import functools

import jax
import jax.numpy as jnp
from jax import lax
from jax.experimental import pallas as pl
from jax.experimental.pallas import tpu as pltpu
from jax.sharding import PartitionSpec as P

HEAD = 128
CORES = 2
BF = jnp.bfloat16
F32 = jnp.float32
MESH = pl.DeviceIdType.MESH


def kernel(
    n_sp, n_tp, per_head, pad,
    tok_in, wk_in, wv_in, shift_in, wg, bias,
    cm_out, norm_out, max_out,
    tok, wk, wv, far_w, shift, shift_in2, acc_k, acc_v, gates, gate_rows, kp, vp,
    stats, stat_own, norms, norm_own, pair_in, pair_own, st, rs, final, cm,
    tok_sem, far_sem, local_sem, shift_sem, stat_sem, norm_sem, pair_sem, rs_sem, cm_sem,
    send_sem,
):
    s = lax.axis_index("sp")
    t = lax.axis_index("tp")
    half = n_tp // 2
    prompt = t // half
    other = 1 - prompt
    mate = lax.rem(t + half, n_tp)
    z, core = s // CORES, lax.rem(s, CORES)
    n_z = n_sp // CORES
    seg, width = tok.shape[1], tok.shape[2]
    cols = wk.shape[2]
    sends = []
    count = [0]

    def remote(src, dst, recv, sp_to, tp_to):
        k = count[0]
        count[0] += 1
        return pltpu.make_async_remote_copy(
            src_ref=src, dst_ref=dst, send_sem=send_sem.at[k], recv_sem=recv,
            device_id=(sp_to, tp_to), device_id_type=MESH,
        )

    def send(src, dst, recv, sp_to, tp_to):
        copy = remote(src, dst, recv, sp_to, tp_to)
        copy.start()
        sends.append((None, copy))

    def send_if(cond, src, dst, recv, sp_to, tp_to):
        copy = remote(src, dst, recv, sp_to, tp_to)

        @pl.when(cond)
        def _():
            copy.start()

        sends.append((cond, copy))

    def arrived(ref, sem):
        pltpu.make_async_copy(ref, ref, sem).wait()

    barrier = pltpu.get_barrier_semaphore()
    greeted = 0
    for d in range(1, n_tp):
        pl.semaphore_signal(barrier, inc=1, device_id=(s, lax.rem(t + d, n_tp)), device_id_type=MESH)
        greeted += 1
    for d in range(1, n_sp):
        for column in (t, mate):
            pl.semaphore_signal(
                barrier, inc=1, device_id=(lax.rem(s + d, n_sp), column), device_id_type=MESH
            )
            greeted += 1

    loads = []

    def load(src, dst):
        copy = pltpu.make_async_copy(src, dst, local_sem.at[len(loads)])
        copy.start()
        loads.append(copy)

    load(tok_in.at[prompt], tok.at[t])
    load(wk_in, wk)
    load(wv_in, wv)
    load(shift_in.at[prompt], shift)
    pl.semaphore_wait(barrier, greeted)

    uneven = n_z >= 4
    slots = 5 if uneven else 4
    units = 2 * n_z

    def flag(cond):
        return jnp.where(cond, 1, 0)

    def share(o):
        if not uneven:
            return 4, 4 * o
        extra = flag(o == 0) + flag(o == n_z - 1) - flag(o == 1) - flag(o == n_z - 2)
        return 4 + extra, 4 * o + flag(o == 1) - flag(o == n_z - 1)

    def slab_of(i):
        i = jnp.clip(i, 0, 2 * units - 1)
        return i // units, lax.rem(i, units) * CORES + core

    sibling = z * CORES + 1 - core
    above = jnp.minimum(z + 1, n_z - 1) * CORES + core
    below = jnp.maximum(z - 1, 0) * CORES + core
    own_count, own_start = share(z)
    for j in range(slots):
        kv, at = slab_of(own_start + j)
        for which, source in ((0, wk_in), (1, wv_in)):
            send_if(
                (j < own_count) & (kv == which), source.at[at], far_w.at[which, at],
                far_sem.at[which, at], s, mate,
            )

    send(shift_in.at[other], shift_in2, shift_sem, s, mate)
    chunks = tok_sem.shape[1]
    rows = seg // chunks
    peers = [prompt * half + lax.rem(t + d, half) for d in range(1, half)]
    for part in range(chunks):
        span = pl.ds(part * rows, rows)
        send(tok_in.at[other, span], tok.at[t, span], tok_sem.at[t, part], s, mate)
        for peer in peers:
            send(tok_in.at[prompt, span], tok.at[t, span], tok_sem.at[t, part], s, peer)

    def relay_tokens(part):
        span = pl.ds(part * rows, rows)
        arrived(tok.at[mate, span], tok_sem.at[mate, part])
        for peer in peers:
            send(tok.at[mate, span], tok.at[mate, span], tok_sem.at[mate, part], s, peer)

    def pass_on(o, j, up, down):
        number, start = share(o)
        valid = (o >= 0) & (o < n_z) & (j < number)
        kv, at = slab_of(start + j)
        here, sem = far_w.at[kv, at], far_sem.at[kv, at]

        @pl.when(valid)
        def _():
            arrived(here, sem)

        if up:
            send_if(valid & (z + 1 < n_z), here, here, sem, above, t)
        if down:
            send_if(valid & (z > 0), here, here, sem, below, t)
        send_if(valid, here, here, sem, sibling, t)

    def stage(r, j):
        if r == 0:
            pass_on(z, j, True, True)
        else:
            pass_on(z - r, j, True, False)
            pass_on(z + r, j, False, True)

    tile = 256 if seg % 256 == 0 else seg
    tiles = seg // tile
    per_slot = wk.shape[0] // n_tp

    def weight_rows(ref, q):
        return ref[pl.ds(q * per_slot, per_slot)].reshape(width, cols)

    def project(q, first):
        @pl.loop(0, tiles)
        def _(i):
            span = pl.ds(pl.multiple_of(i * tile, tile), tile)
            x = tok[q, span, :]
            ak = jnp.dot(x, weight_rows(wk, q), preferred_element_type=F32)
            av = jnp.dot(x, weight_rows(wv, q), preferred_element_type=F32)
            if first:
                acc_k[span, :] = ak
                acc_v[span, :] = av
            else:
                acc_k[span, :] += ak
                acc_v[span, :] += av

        g = lax.dot_general(wg[:, pl.ds(pl.multiple_of(q * width, width), width)], tok[q], (((1,), (1,)), ((), ())), preferred_element_type=F32)
        gates[...] = g if first else gates[...] + g

    stage(0, 0)
    for copy in loads:
        copy.wait()
    project(t, True)

    def peer_tokens(q):
        for part in range(chunks):
            span = pl.ds(part * rows, rows)
            arrived(tok.at[q, span], tok_sem.at[q, part])
        project(q, False)

    order = sorted(
        ((r, j) for r in range(n_z) for j in range(slots)), key=lambda x: (x[0] + x[1], x[0])
    )
    place = [int(len(order) * (0.5 + 0.4 * part / chunks)) for part in range(chunks)]
    for k, (r, j) in enumerate(order):
        if (r, j) != (0, 0):
            stage(r, j)
        for part in range(chunks):
            if place[part] == k:
                relay_tokens(part)
        if k == place[chunks // 2]:
            for peer in peers:
                peer_tokens(peer)
    project(mate, False)
    for peer in peers:
        peer_tokens(lax.rem(peer + half, n_tp))

    arrived(shift_in2, shift_sem)
    heads_all = n_tp * per_head
    eye = lax.broadcasted_iota(jnp.int32, (heads_all, heads_all), 0) == lax.broadcasted_iota(
        jnp.int32, (heads_all, heads_all), 1
    )
    gate_rows[...] = jnp.zeros_like(gate_rows)
    for g in range(4):
        rows_g = gates[g * heads_all : (g + 1) * heads_all, :]
        if g % 2:
            rows_g = rows_g + jnp.sum(
                jnp.where(eye, bias[g // 2 : g // 2 + 1, :], 0.0), axis=1, keepdims=True
            )
        for k in range(n_tp):
            @pl.when(t == k)
            def _():
                gate_rows[g, 0:per_head, :] = rows_g[k * per_head : (k + 1) * per_head]

            @pl.when(mate == k)
            def _():
                gate_rows[g, per_head : 2 * per_head, :] = rows_g[k * per_head : (k + 1) * per_head]

    def shifts(g):
        parts = [shift[g], shift_in2[g]]
        if pad > 2 * per_head:
            parts.append(jnp.zeros((pad - 2 * per_head, seg), F32))
        return jnp.concatenate(parts, axis=0)

    lane = lax.broadcasted_iota(jnp.int32, (pad, seg), 1)

    def log_sigmoid(v):
        return jnp.minimum(v, 0.0) - jnp.log1p(jnp.exp(-jnp.abs(v)))

    def climb(v):
        step = 1
        while step < seg:
            v = v + jnp.where(lane >= step, pltpu.roll(v, step, 1), 0.0)
            step *= 2
        return v

    in_f = gate_rows[0] + shifts(0)
    fo_f = log_sigmoid(gate_rows[1]) + shifts(1)
    in_b = gate_rows[2] + shifts(2)
    fo_b = log_sigmoid(gate_rows[3]) + shifts(3)
    total_f = jnp.sum(fo_f, axis=1, keepdims=True)
    total_b = jnp.sum(fo_b, axis=1, keepdims=True)
    w_f = total_f - climb(fo_f) + in_f
    w_b = climb(fo_b) - fo_b + in_b
    top_f = jnp.max(w_f, axis=1, keepdims=True)
    top_b = jnp.max(w_b, axis=1, keepdims=True)
    first_lane = lax.broadcasted_iota(jnp.int32, (pad, HEAD), 1) == 0
    stat_own[0] = jnp.where(first_lane, top_f, total_f)
    stat_own[1] = jnp.where(first_lane, top_b, total_b)
    for d in range(1, n_sp):
        to = lax.rem(s + d, n_sp)
        send(stat_own, stats.at[s], stat_sem.at[s], to, t)

    def far(held, dest):
        @pl.loop(0, tiles)
        def _(i):
            span = pl.ds(pl.multiple_of(i * tile, tile), tile)
            total = jnp.zeros((tile, cols), F32)
            for q in range(n_tp):
                total += jnp.dot(tok[q, span, :], weight_rows(held, q), preferred_element_type=F32)
            dest[span, :] = total.astype(BF)

    def swapped(kv):
        for k in range(units):
            got = k * CORES + 1 - core
            arrived(far_w.at[kv, got], far_sem.at[kv, got])

    swapped(0)
    far(far_w.at[0], kp)

    stats[s] = stat_own[...]
    for d in range(1, n_sp):
        frm = lax.rem(s + d, n_sp)
        arrived(stats.at[frm], stat_sem.at[frm])

    everyone = [stats[k] for k in range(n_sp)]
    total_all = [0.0, 0.0]
    after = [None] * n_sp
    running = jnp.zeros((pad, 1), F32)
    for k in reversed(range(n_sp)):
        after[k] = running
        running = running + everyone[k][0][:, 1:2]
    total_all[0] = running
    before = [None] * n_sp
    running = jnp.zeros((pad, 1), F32)
    for k in range(n_sp):
        before[k] = running
        running = running + everyone[k][1][:, 1:2]
    total_all[1] = running
    max_f, max_b = total_all
    passed_f = jnp.zeros((pad, 1), F32)
    passed_b = jnp.zeros((pad, 1), F32)
    for k in range(n_sp):
        max_f = jnp.maximum(max_f, everyone[k][0][:, 0:1] + after[k])
        max_b = jnp.maximum(max_b, everyone[k][1][:, 0:1] + before[k])
        passed_f = jnp.where(s == k, after[k], passed_f)
        passed_b = jnp.where(s == k, before[k], passed_b)
    scale_f = jnp.exp(w_f + (passed_f - max_f)) * HEAD**-0.5
    scale_b = jnp.exp(w_b + (passed_b - max_b)) * HEAD**-0.5
    both = jnp.concatenate([scale_f, scale_b], axis=0)
    scale_hi = both.astype(BF)
    scale_lo = (both - scale_hi.astype(F32)).astype(BF)

    block = st.shape[0] // n_sp
    row_of = lax.broadcasted_iota(jnp.int32, (2 * pad, HEAD), 0)
    norm_own[...] = jnp.zeros_like(norm_own)

    def head_state(index, k_h, v_h):
        k_t = k_h.astype(F32).T
        both_t = jnp.concatenate(
            [k_t * scale_f[index : index + 1, :], k_t * scale_b[index : index + 1, :]], axis=0
        ).astype(BF)
        st[index * 2 * HEAD : (index + 1) * 2 * HEAD, :] = jnp.dot(
            both_t, v_h, preferred_element_type=F32
        ).astype(BF)
        n = jnp.dot(scale_hi, k_h, preferred_element_type=F32) + jnp.dot(
            scale_lo, k_h, preferred_element_type=F32
        )
        mine = (row_of == index) | (row_of == index + pad)
        norm_own[...] = jnp.where(mine, n, norm_own[...])

    def scatter(side):
        for k in range(n_sp // 2):
            owner = side * (n_sp // 2) + k
            send_if(
                s != owner,
                st.at[pl.ds(owner * block, block)],
                rs.at[s], rs_sem.at[s], jnp.where(s == owner, sibling, owner), t,
            )

    for h in range(per_head):
        at = slice(h * HEAD, (h + 1) * HEAD)
        head_state(h, acc_k[:, at].astype(BF), acc_v[:, at].astype(BF))
    scatter(0)

    swapped(1)
    far(far_w.at[1], vp)
    for h in range(per_head):
        at = slice(h * HEAD, (h + 1) * HEAD)
        head_state(per_head + h, kp[:, at], vp[:, at])
    scatter(1)
    for d in range(1, n_sp):
        to = lax.rem(s + d, n_sp)
        send(norm_own, norms.at[s], norm_sem.at[s], to, t)
    norms[s] = norm_own[...]

    summed = st[pl.ds(pl.multiple_of(s * block, block), block), :].astype(F32)
    for d in range(1, n_sp):
        frm = lax.rem(s + d, n_sp)
        arrived(rs.at[frm], rs_sem.at[frm])
        summed = summed + rs[frm].astype(F32)
    final[...] = summed.astype(BF)

    piece = min(block, HEAD)
    mine_side = s < n_sp // 2
    column = jnp.where(mine_side, t, mate)
    for c in range(block // piece):
        start = s * block + c * piece
        head = lax.rem(start // (2 * HEAD), per_head)
        direction = lax.rem(start // HEAD, 2)
        inner = pl.ds(pl.multiple_of(lax.rem(start, HEAD), piece), piece)
        src = final.at[pl.ds(c * piece, piece)]
        dst = cm.at[prompt, direction, head, inner]
        for d in range(1, n_sp):
            send(src, dst, cm_sem.at[prompt], lax.rem(s + d, n_sp), column)
        keep = pltpu.make_async_copy(src, dst, cm_sem.at[prompt])

        @pl.when(mine_side)
        def _():
            keep.start()

        send_if(jnp.logical_not(mine_side), src, dst, cm_sem.at[prompt], s, mate)

    total_norm = jnp.zeros((2 * pad, HEAD), F32)
    for d in range(1, n_sp):
        frm = lax.rem(s + d, n_sp)
        arrived(norms.at[frm], norm_sem.at[frm])
    for k in range(n_sp):
        total_norm = total_norm + norms[k]
    pair_own[0] = total_norm
    pair_own[1, 0:pad, :] = jnp.broadcast_to(max_f, (pad, HEAD))
    pair_own[1, pad : 2 * pad, :] = jnp.broadcast_to(max_b, (pad, HEAD))
    send(pair_own, pair_in, pair_sem, s, mate)
    for j in range(2):
        norm_out[prompt, j] = pair_own[0, j * pad : j * pad + per_head, :]
        max_out[prompt, j] = pair_own[1, j * pad : j * pad + per_head, :]
    arrived(pair_in, pair_sem)
    for j in range(2):
        lo = j * pad + per_head
        norm_out[other, j] = pair_in[0, lo : lo + per_head, :]
        max_out[other, j] = pair_in[1, lo : lo + per_head, :]

    for b in range(2):
        arrived(cm.at[b], cm_sem.at[b])
    store = pltpu.make_async_copy(cm, cm_out, local_sem.at[len(loads)])
    store.start()
    for cond, copy in sends:
        if cond is None:
            copy.wait_send()
        else:
            pl.when(cond)(copy.wait_send)
    store.wait()


def finish(cm, norm, top, query, cm_out, norm_out, max_out, read_out):
    seqs, _, per_head = norm.shape[:3]
    row = lax.broadcasted_iota(jnp.int32, (per_head, HEAD), 0)
    diagonal = row == lax.broadcasted_iota(jnp.int32, (per_head, HEAD), 1)
    cm_out[...] = cm[...]
    norm_out[...] = norm[...]
    for b in range(seqs):
        for j in range(2):
            line = jnp.sum(jnp.where(diagonal, top[b, j], 0.0), axis=0, keepdims=True)
            max_out[b, j : j + 1, :] = line[:, 0:per_head]
        for h in range(per_head):
            at = slice(h * HEAD, (h + 1) * HEAD)
            q = query[b, :, at]
            q_f = q.astype(F32)
            total = jnp.zeros(q_f.shape, F32)
            for j in range(2):
                num = jnp.dot(q, cm[b, j, h], preferred_element_type=F32)
                den = jnp.sum(q_f * norm[b, j, h : h + 1, :], axis=1, keepdims=True)
                total = total + num / jnp.maximum(jnp.abs(den), 1.0)
            read_out[b, :, at] = total.astype(BF)


def on_device(n_sp, n_tp, tokens, w_key, w_value, w_gate, forget_bias, log_shift, new_query):
    seqs, seg, width = tokens.shape
    depth_all, cols = w_key.shape
    per_head = cols // HEAD
    pad = -(-2 * per_head // 8) * 8
    heads_all = w_gate.shape[2]
    gate_t = w_gate.transpose(1, 2, 0).reshape(4 * heads_all, depth_all)
    slabs = (2 * n_sp, depth_all // (2 * n_sp), cols)
    state_rows = 2 * per_head * 2 * HEAD
    block = state_rows // n_sp
    n_z = n_sp // CORES
    half = n_tp // 2
    chunks = 4
    n_send = (
        10 + 1 + chunks * (2 * half - 1) + 5 * 3 + (n_z - 1) * 5 * 4
        + 3 * (n_sp - 1) + n_sp + max(1, block // HEAD) * n_sp + 4
    )
    vmem = pltpu.VMEM
    dma = pltpu.SemaphoreType.DMA
    new = new_query.shape[1]
    any_spec = pl.BlockSpec(memory_space=pl.ANY)
    vm_spec = pl.BlockSpec(memory_space=vmem)
    cm, norm, top = pl.pallas_call(
        functools.partial(kernel, n_sp, n_tp, per_head, pad),
        out_shape=(
            jax.ShapeDtypeStruct((seqs, 2, per_head, HEAD, HEAD), BF),
            jax.ShapeDtypeStruct((seqs, 2, per_head, HEAD), F32),
            jax.ShapeDtypeStruct((seqs, 2, per_head, HEAD), F32),
        ),
        in_specs=[any_spec] * 4 + [vm_spec] * 2,
        out_specs=(any_spec, vm_spec, vm_spec),
        scratch_shapes=[
            vmem((n_tp, seg, width), BF),
            vmem(slabs, BF), vmem(slabs, BF), vmem((2,) + slabs, BF),
            vmem((4, per_head, seg), F32), vmem((4, per_head, seg), F32),
            vmem((seg, cols), F32), vmem((seg, cols), F32), vmem((4 * heads_all, seg), F32),
            vmem((4, pad, seg), F32),
            vmem((seg, cols), BF), vmem((seg, cols), BF),
            vmem((n_sp, 2, pad, HEAD), F32), vmem((2, pad, HEAD), F32),
            vmem((n_sp, 2 * pad, HEAD), F32), vmem((2 * pad, HEAD), F32),
            vmem((2, 2 * pad, HEAD), F32), vmem((2, 2 * pad, HEAD), F32),
            vmem((state_rows, HEAD), BF), vmem((n_sp, block, HEAD), BF), vmem((block, HEAD), BF),
            vmem((seqs, 2, per_head, HEAD, HEAD), BF),
            dma((n_tp, chunks)), dma((2, 2 * n_sp)), dma((6,)), dma, dma((n_sp,)), dma((n_sp,)),
            dma, dma((n_sp,)), dma((2,)), dma((n_send,)),
        ],
        compiler_params=pltpu.CompilerParams(
            collective_id=0, has_side_effects=True, vmem_limit_bytes=60 * 2**20
        ),
    )(
        tokens, w_key.reshape(slabs), w_value.reshape(slabs), log_shift, gate_t, forget_bias
    )
    return pl.pallas_call(
        finish,
        out_shape=(
            jax.ShapeDtypeStruct(cm.shape, BF),
            jax.ShapeDtypeStruct(norm.shape, F32),
            jax.ShapeDtypeStruct(norm.shape[:3], F32),
            jax.ShapeDtypeStruct((seqs, new, cols), BF),
        ),
        in_specs=[vm_spec] * 4,
        out_specs=(vm_spec,) * 4,
    )(cm, norm, top, new_query)


def solution(mesh):
    return jax.shard_map(
        functools.partial(on_device, mesh.shape["sp"], mesh.shape["tp"]),
        mesh=mesh,
        in_specs=(
            P(None, "sp", "tp"),
            P(None, "tp"),
            P(None, "tp"),
            P(),
            P(),
            P(None, None, "tp", "sp"),
            P(None, "sp", "tp"),
        ),
        out_specs=(
            P(None, None, "tp", None, None),
            P(None, None, "tp", None),
            P(None, None, "tp"),
            P(None, "sp", "tp"),
        ),
        check_vma=False,
    )
```

```python
import functools

import jax
import jax.numpy as jnp
from jax import lax
from jax.experimental import pallas as pl
from jax.experimental.pallas import tpu as pltpu
from jax.sharding import PartitionSpec as P

HEAD = 128
CORES = 2
BF = jnp.bfloat16
F32 = jnp.float32
MESH = pl.DeviceIdType.MESH


def kernel(
    n_sp, n_tp, per_head, pad,
    tok_in, wk_in, wv_in, shift_in, wg, bias,
    cm_out, norm_out, max_out,
    tok, wk, wv, far_w, shift, shift_in2, acc_k, acc_v, gates, gate_rows, kp, vp,
    stats, stat_own, norms, norm_own, pair_in, pair_own, st, chip, rs, final, cm,
    tok_sem, far_sem, local_sem, shift_sem, stat_sem, norm_sem, pair_sem, chip_sem, rs_sem, cm_sem,
    send_sem,
):
    s = lax.axis_index("sp")
    t = lax.axis_index("tp")
    half = n_tp // 2
    prompt = t // half
    other = 1 - prompt
    mate = lax.rem(t + half, n_tp)
    z, core = s // CORES, lax.rem(s, CORES)
    n_z = n_sp // CORES
    seg, width = tok.shape[1], tok.shape[2]
    cols = wk.shape[2]
    sends = []
    count = [0]

    def remote(src, dst, recv, sp_to, tp_to):
        k = count[0]
        count[0] += 1
        return pltpu.make_async_remote_copy(
            src_ref=src, dst_ref=dst, send_sem=send_sem.at[k], recv_sem=recv,
            device_id=(sp_to, tp_to), device_id_type=MESH,
        )

    def send(src, dst, recv, sp_to, tp_to):
        copy = remote(src, dst, recv, sp_to, tp_to)
        copy.start()
        sends.append((None, copy))

    def send_if(cond, src, dst, recv, sp_to, tp_to):
        copy = remote(src, dst, recv, sp_to, tp_to)

        @pl.when(cond)
        def _():
            copy.start()

        sends.append((cond, copy))

    def arrived(ref, sem):
        pltpu.make_async_copy(ref, ref, sem).wait()

    barrier = pltpu.get_barrier_semaphore()
    greeted = 0
    for d in range(1, n_tp):
        pl.semaphore_signal(barrier, inc=1, device_id=(s, lax.rem(t + d, n_tp)), device_id_type=MESH)
        greeted += 1
    for d in range(1, n_sp):
        for column in (t, mate):
            pl.semaphore_signal(
                barrier, inc=1, device_id=(lax.rem(s + d, n_sp), column), device_id_type=MESH
            )
            greeted += 1

    loads = []

    def load(src, dst):
        copy = pltpu.make_async_copy(src, dst, local_sem.at[len(loads)])
        copy.start()
        loads.append(copy)

    load(tok_in.at[prompt], tok.at[t])
    load(wk_in, wk)
    load(wv_in, wv)
    load(shift_in.at[prompt], shift)
    pl.semaphore_wait(barrier, greeted)

    uneven = n_z >= 4
    slots = 5 if uneven else 4
    units = 2 * n_z

    def flag(cond):
        return jnp.where(cond, 1, 0)

    def share(o):
        if not uneven:
            return 4, 4 * o
        extra = flag(o == 0) + flag(o == n_z - 1) - flag(o == 1) - flag(o == n_z - 2)
        return 4 + extra, 4 * o + flag(o == 1) - flag(o == n_z - 1)

    def slab_of(i):
        i = jnp.clip(i, 0, 2 * units - 1)
        return i // units, lax.rem(i, units) * CORES + core

    sibling = z * CORES + 1 - core
    above = jnp.minimum(z + 1, n_z - 1) * CORES + core
    below = jnp.maximum(z - 1, 0) * CORES + core
    own_count, own_start = share(z)
    for j in range(slots):
        kv, at = slab_of(own_start + j)
        for which, source in ((0, wk_in), (1, wv_in)):
            send_if(
                (j < own_count) & (kv == which), source.at[at], far_w.at[which, at],
                far_sem.at[which, at], s, mate,
            )

    send(shift_in.at[other], shift_in2, shift_sem, s, mate)
    chunks = tok_sem.shape[1]
    rows = seg // chunks
    peers = [prompt * half + lax.rem(t + d, half) for d in range(1, half)]
    for part in range(chunks):
        span = pl.ds(part * rows, rows)
        send(tok_in.at[other, span], tok.at[t, span], tok_sem.at[t, part], s, mate)
        for peer in peers:
            send(tok_in.at[prompt, span], tok.at[t, span], tok_sem.at[t, part], s, peer)

    def relay_tokens(part):
        span = pl.ds(part * rows, rows)
        arrived(tok.at[mate, span], tok_sem.at[mate, part])
        for peer in peers:
            send(tok.at[mate, span], tok.at[mate, span], tok_sem.at[mate, part], s, peer)

    def pass_on(o, j, up, down):
        number, start = share(o)
        valid = (o >= 0) & (o < n_z) & (j < number)
        kv, at = slab_of(start + j)
        here, sem = far_w.at[kv, at], far_sem.at[kv, at]

        @pl.when(valid)
        def _():
            arrived(here, sem)

        if up:
            send_if(valid & (z + 1 < n_z), here, here, sem, above, t)
        if down:
            send_if(valid & (z > 0), here, here, sem, below, t)
        send_if(valid, here, here, sem, sibling, t)

    def stage(r, j):
        if r == 0:
            pass_on(z, j, True, True)
        else:
            pass_on(z - r, j, True, False)
            pass_on(z + r, j, False, True)

    tile = 256 if seg % 256 == 0 else seg
    tiles = seg // tile
    per_slot = wk.shape[0] // n_tp

    def weight_rows(ref, q):
        return ref[pl.ds(q * per_slot, per_slot)].reshape(width, cols)

    def project(q, first):
        @pl.loop(0, tiles)
        def _(i):
            span = pl.ds(pl.multiple_of(i * tile, tile), tile)
            x = tok[q, span, :]
            ak = jnp.dot(x, weight_rows(wk, q), preferred_element_type=F32)
            av = jnp.dot(x, weight_rows(wv, q), preferred_element_type=F32)
            if first:
                acc_k[span, :] = ak
                acc_v[span, :] = av
            else:
                acc_k[span, :] += ak
                acc_v[span, :] += av

        g = lax.dot_general(wg[:, pl.ds(pl.multiple_of(q * width, width), width)], tok[q], (((1,), (1,)), ((), ())), preferred_element_type=F32)
        gates[...] = g if first else gates[...] + g

    stage(0, 0)
    for copy in loads:
        copy.wait()
    project(t, True)

    def peer_tokens(q):
        for part in range(chunks):
            span = pl.ds(part * rows, rows)
            arrived(tok.at[q, span], tok_sem.at[q, part])
        project(q, False)

    order = sorted(
        ((r, j) for r in range(n_z) for j in range(slots)), key=lambda x: (x[0] + x[1], x[0])
    )
    place = [int(len(order) * (0.5 + 0.4 * part / chunks)) for part in range(chunks)]
    for k, (r, j) in enumerate(order):
        if (r, j) != (0, 0):
            stage(r, j)
        for part in range(chunks):
            if place[part] == k:
                relay_tokens(part)
        if k == place[chunks // 2]:
            for peer in peers:
                peer_tokens(peer)
    project(mate, False)
    for peer in peers:
        peer_tokens(lax.rem(peer + half, n_tp))

    arrived(shift_in2, shift_sem)
    heads_all = n_tp * per_head
    eye = lax.broadcasted_iota(jnp.int32, (heads_all, heads_all), 0) == lax.broadcasted_iota(
        jnp.int32, (heads_all, heads_all), 1
    )
    gate_rows[...] = jnp.zeros_like(gate_rows)
    for g in range(4):
        rows_g = gates[g * heads_all : (g + 1) * heads_all, :]
        if g % 2:
            rows_g = rows_g + jnp.sum(
                jnp.where(eye, bias[g // 2 : g // 2 + 1, :], 0.0), axis=1, keepdims=True
            )
        for k in range(n_tp):
            @pl.when(t == k)
            def _():
                gate_rows[g, 0:per_head, :] = rows_g[k * per_head : (k + 1) * per_head]

            @pl.when(mate == k)
            def _():
                gate_rows[g, per_head : 2 * per_head, :] = rows_g[k * per_head : (k + 1) * per_head]

    def shifts(g):
        parts = [shift[g], shift_in2[g]]
        if pad > 2 * per_head:
            parts.append(jnp.zeros((pad - 2 * per_head, seg), F32))
        return jnp.concatenate(parts, axis=0)

    lane = lax.broadcasted_iota(jnp.int32, (pad, seg), 1)

    def log_sigmoid(v):
        return jnp.minimum(v, 0.0) - jnp.log1p(jnp.exp(-jnp.abs(v)))

    def climb(v):
        step = 1
        while step < seg:
            v = v + jnp.where(lane >= step, pltpu.roll(v, step, 1), 0.0)
            step *= 2
        return v

    in_f = gate_rows[0] + shifts(0)
    fo_f = log_sigmoid(gate_rows[1]) + shifts(1)
    in_b = gate_rows[2] + shifts(2)
    fo_b = log_sigmoid(gate_rows[3]) + shifts(3)
    total_f = jnp.sum(fo_f, axis=1, keepdims=True)
    total_b = jnp.sum(fo_b, axis=1, keepdims=True)
    w_f = total_f - climb(fo_f) + in_f
    w_b = climb(fo_b) - fo_b + in_b
    top_f = jnp.max(w_f, axis=1, keepdims=True)
    top_b = jnp.max(w_b, axis=1, keepdims=True)
    first_lane = lax.broadcasted_iota(jnp.int32, (pad, HEAD), 1) == 0
    stat_own[0] = jnp.where(first_lane, top_f, total_f)
    stat_own[1] = jnp.where(first_lane, top_b, total_b)
    for d in range(1, n_sp):
        to = lax.rem(s + d, n_sp)
        send(stat_own, stats.at[s], stat_sem.at[s], to, t)

    def far(held, dest):
        @pl.loop(0, tiles)
        def _(i):
            span = pl.ds(pl.multiple_of(i * tile, tile), tile)
            total = jnp.zeros((tile, cols), F32)
            for q in range(n_tp):
                total += jnp.dot(tok[q, span, :], weight_rows(held, q), preferred_element_type=F32)
            dest[span, :] = total.astype(BF)

    def swapped(kv):
        for k in range(units):
            got = k * CORES + 1 - core
            arrived(far_w.at[kv, got], far_sem.at[kv, got])

    swapped(0)
    far(far_w.at[0], kp)

    stats[s] = stat_own[...]
    for d in range(1, n_sp):
        frm = lax.rem(s + d, n_sp)
        arrived(stats.at[frm], stat_sem.at[frm])

    everyone = [stats[k] for k in range(n_sp)]
    total_all = [0.0, 0.0]
    after = [None] * n_sp
    running = jnp.zeros((pad, 1), F32)
    for k in reversed(range(n_sp)):
        after[k] = running
        running = running + everyone[k][0][:, 1:2]
    total_all[0] = running
    before = [None] * n_sp
    running = jnp.zeros((pad, 1), F32)
    for k in range(n_sp):
        before[k] = running
        running = running + everyone[k][1][:, 1:2]
    total_all[1] = running
    max_f, max_b = total_all
    passed_f = jnp.zeros((pad, 1), F32)
    passed_b = jnp.zeros((pad, 1), F32)
    for k in range(n_sp):
        max_f = jnp.maximum(max_f, everyone[k][0][:, 0:1] + after[k])
        max_b = jnp.maximum(max_b, everyone[k][1][:, 0:1] + before[k])
        passed_f = jnp.where(s == k, after[k], passed_f)
        passed_b = jnp.where(s == k, before[k], passed_b)
    scale_f = jnp.exp(w_f + (passed_f - max_f)) * HEAD**-0.5
    scale_b = jnp.exp(w_b + (passed_b - max_b)) * HEAD**-0.5
    both = jnp.concatenate([scale_f, scale_b], axis=0)
    scale_hi = both.astype(BF)
    scale_lo = (both - scale_hi.astype(F32)).astype(BF)

    block = st.shape[0] // n_sp
    row_of = lax.broadcasted_iota(jnp.int32, (2 * pad, HEAD), 0)
    norm_own[...] = jnp.zeros_like(norm_own)

    def head_state(index, k_h, v_h):
        k_t = k_h.astype(F32).T
        both_t = jnp.concatenate(
            [k_t * scale_f[index : index + 1, :], k_t * scale_b[index : index + 1, :]], axis=0
        ).astype(BF)
        st[index * 2 * HEAD : (index + 1) * 2 * HEAD, :] = jnp.dot(
            both_t, v_h, preferred_element_type=F32
        ).astype(BF)
        n = jnp.dot(scale_hi, k_h, preferred_element_type=F32) + jnp.dot(
            scale_lo, k_h, preferred_element_type=F32
        )
        mine = (row_of == index) | (row_of == index + pad)
        norm_own[...] = jnp.where(mine, n, norm_own[...])

    def block_at(owner):
        return pl.ds(pl.multiple_of(owner * block, block), block)

    def scatter(side):
        quarter = n_sp // 4
        for m in range(quarter):
            theirs = side * (n_sp // 2) + m * CORES + 1 - core
            slot = side * quarter + m
            send(st.at[block_at(theirs)], chip.at[slot], chip_sem.at[slot], sibling, t)
        for m in range(quarter):
            owner = side * (n_sp // 2) + m * CORES + core
            slot = side * quarter + m
            arrived(chip.at[slot], chip_sem.at[slot])
            st[block_at(owner), :] = (
                st[block_at(owner), :].astype(F32) + chip[slot].astype(F32)
            ).astype(BF)
            send_if(
                s != owner, st.at[block_at(owner)], rs.at[z], rs_sem.at[z],
                jnp.where(s == owner, sibling, owner), t,
            )

    for h in range(per_head):
        at = slice(h * HEAD, (h + 1) * HEAD)
        head_state(h, acc_k[:, at].astype(BF), acc_v[:, at].astype(BF))
    scatter(0)

    swapped(1)
    far(far_w.at[1], vp)
    for h in range(per_head):
        at = slice(h * HEAD, (h + 1) * HEAD)
        head_state(per_head + h, kp[:, at], vp[:, at])
    scatter(1)
    for d in range(1, n_sp):
        to = lax.rem(s + d, n_sp)
        send(norm_own, norms.at[s], norm_sem.at[s], to, t)
    norms[s] = norm_own[...]

    summed = st[pl.ds(pl.multiple_of(s * block, block), block), :].astype(F32)
    for d in range(1, n_z):
        frm = lax.rem(z + d, n_z)
        arrived(rs.at[frm], rs_sem.at[frm])
        summed = summed + rs[frm].astype(F32)
    final[...] = summed.astype(BF)

    piece = min(block, HEAD)
    mine_side = s < n_sp // 2
    column = jnp.where(mine_side, t, mate)
    for c in range(block // piece):
        start = s * block + c * piece
        head = lax.rem(start // (2 * HEAD), per_head)
        direction = lax.rem(start // HEAD, 2)
        inner = pl.ds(pl.multiple_of(lax.rem(start, HEAD), piece), piece)
        src = final.at[pl.ds(c * piece, piece)]
        dst = cm.at[prompt, direction, head, inner]
        for d in range(1, n_sp):
            send(src, dst, cm_sem.at[prompt], lax.rem(s + d, n_sp), column)
        keep = pltpu.make_async_copy(src, dst, cm_sem.at[prompt])

        @pl.when(mine_side)
        def _():
            keep.start()

        send_if(jnp.logical_not(mine_side), src, dst, cm_sem.at[prompt], s, mate)

    total_norm = jnp.zeros((2 * pad, HEAD), F32)
    for d in range(1, n_sp):
        frm = lax.rem(s + d, n_sp)
        arrived(norms.at[frm], norm_sem.at[frm])
    for k in range(n_sp):
        total_norm = total_norm + norms[k]
    pair_own[0] = total_norm
    pair_own[1, 0:pad, :] = jnp.broadcast_to(max_f, (pad, HEAD))
    pair_own[1, pad : 2 * pad, :] = jnp.broadcast_to(max_b, (pad, HEAD))
    send(pair_own, pair_in, pair_sem, s, mate)
    for j in range(2):
        norm_out[prompt, j] = pair_own[0, j * pad : j * pad + per_head, :]
        max_out[prompt, j] = pair_own[1, j * pad : j * pad + per_head, :]
    arrived(pair_in, pair_sem)
    for j in range(2):
        lo = j * pad + per_head
        norm_out[other, j] = pair_in[0, lo : lo + per_head, :]
        max_out[other, j] = pair_in[1, lo : lo + per_head, :]

    for b in range(2):
        arrived(cm.at[b], cm_sem.at[b])
    store = pltpu.make_async_copy(cm, cm_out, local_sem.at[len(loads)])
    store.start()
    for cond, copy in sends:
        if cond is None:
            copy.wait_send()
        else:
            pl.when(cond)(copy.wait_send)
    store.wait()


def finish(cm, norm, top, query, cm_out, norm_out, max_out, read_out):
    seqs, _, per_head = norm.shape[:3]
    row = lax.broadcasted_iota(jnp.int32, (per_head, HEAD), 0)
    diagonal = row == lax.broadcasted_iota(jnp.int32, (per_head, HEAD), 1)
    cm_out[...] = cm[...]
    norm_out[...] = norm[...]
    for b in range(seqs):
        for j in range(2):
            line = jnp.sum(jnp.where(diagonal, top[b, j], 0.0), axis=0, keepdims=True)
            max_out[b, j : j + 1, :] = line[:, 0:per_head]
        for h in range(per_head):
            at = slice(h * HEAD, (h + 1) * HEAD)
            q = query[b, :, at]
            q_f = q.astype(F32)
            total = jnp.zeros(q_f.shape, F32)
            for j in range(2):
                num = jnp.dot(q, cm[b, j, h], preferred_element_type=F32)
                den = jnp.sum(q_f * norm[b, j, h : h + 1, :], axis=1, keepdims=True)
                total = total + num / jnp.maximum(jnp.abs(den), 1.0)
            read_out[b, :, at] = total.astype(BF)


def on_device(n_sp, n_tp, tokens, w_key, w_value, w_gate, forget_bias, log_shift, new_query):
    seqs, seg, width = tokens.shape
    depth_all, cols = w_key.shape
    per_head = cols // HEAD
    pad = -(-2 * per_head // 8) * 8
    heads_all = w_gate.shape[2]
    gate_t = w_gate.transpose(1, 2, 0).reshape(4 * heads_all, depth_all)
    slabs = (2 * n_sp, depth_all // (2 * n_sp), cols)
    state_rows = 2 * per_head * 2 * HEAD
    block = state_rows // n_sp
    n_z = n_sp // CORES
    half = n_tp // 2
    chunks = 4
    n_send = (
        10 + 1 + chunks * (2 * half - 1) + 5 * 3 + (n_z - 1) * 5 * 4
        + 3 * (n_sp - 1) + n_sp + max(1, block // HEAD) * n_sp + 4
    )
    vmem = pltpu.VMEM
    dma = pltpu.SemaphoreType.DMA
    new = new_query.shape[1]
    any_spec = pl.BlockSpec(memory_space=pl.ANY)
    vm_spec = pl.BlockSpec(memory_space=vmem)
    cm, norm, top = pl.pallas_call(
        functools.partial(kernel, n_sp, n_tp, per_head, pad),
        out_shape=(
            jax.ShapeDtypeStruct((seqs, 2, per_head, HEAD, HEAD), BF),
            jax.ShapeDtypeStruct((seqs, 2, per_head, HEAD), F32),
            jax.ShapeDtypeStruct((seqs, 2, per_head, HEAD), F32),
        ),
        in_specs=[any_spec] * 4 + [vm_spec] * 2,
        out_specs=(any_spec, vm_spec, vm_spec),
        scratch_shapes=[
            vmem((n_tp, seg, width), BF),
            vmem(slabs, BF), vmem(slabs, BF), vmem((2,) + slabs, BF),
            vmem((4, per_head, seg), F32), vmem((4, per_head, seg), F32),
            vmem((seg, cols), F32), vmem((seg, cols), F32), vmem((4 * heads_all, seg), F32),
            vmem((4, pad, seg), F32),
            vmem((seg, cols), BF), vmem((seg, cols), BF),
            vmem((n_sp, 2, pad, HEAD), F32), vmem((2, pad, HEAD), F32),
            vmem((n_sp, 2 * pad, HEAD), F32), vmem((2 * pad, HEAD), F32),
            vmem((2, 2 * pad, HEAD), F32), vmem((2, 2 * pad, HEAD), F32),
            vmem((state_rows, HEAD), BF), vmem((n_sp // 2, block, HEAD), BF), vmem((n_z, block, HEAD), BF), vmem((block, HEAD), BF),
            vmem((seqs, 2, per_head, HEAD, HEAD), BF),
            dma((n_tp, chunks)), dma((2, 2 * n_sp)), dma((6,)), dma, dma((n_sp,)), dma((n_sp,)),
            dma, dma((n_sp // 2,)), dma((n_z,)), dma((2,)), dma((n_send,)),
        ],
        compiler_params=pltpu.CompilerParams(
            collective_id=0, has_side_effects=True, vmem_limit_bytes=60 * 2**20
        ),
    )(
        tokens, w_key.reshape(slabs), w_value.reshape(slabs), log_shift, gate_t, forget_bias
    )
    return pl.pallas_call(
        finish,
        out_shape=(
            jax.ShapeDtypeStruct(cm.shape, BF),
            jax.ShapeDtypeStruct(norm.shape, F32),
            jax.ShapeDtypeStruct(norm.shape[:3], F32),
            jax.ShapeDtypeStruct((seqs, new, cols), BF),
        ),
        in_specs=[vm_spec] * 4,
        out_specs=(vm_spec,) * 4,
    )(cm, norm, top, new_query)


def solution(mesh):
    return jax.shard_map(
        functools.partial(on_device, mesh.shape["sp"], mesh.shape["tp"]),
        mesh=mesh,
        in_specs=(
            P(None, "sp", "tp"),
            P(None, "tp"),
            P(None, "tp"),
            P(),
            P(),
            P(None, None, "tp", "sp"),
            P(None, "sp", "tp"),
        ),
        out_specs=(
            P(None, None, "tp", None, None),
            P(None, None, "tp", None),
            P(None, None, "tp"),
            P(None, "sp", "tp"),
        ),
        check_vma=False,
    )
```
